32 devices in a mesh: grp: 2 (over x), ep: 16 (over z, y, core), tp: 1.
Axes of the slice: x: 2, y: 2, z: 4, core: 2. Of those that a mesh axis runs over, the one named last changes fastest.
Arguments:
- tokens: bfloat16 [2048, 1024], P(('grp', 'ep')), parts along dimension 0, may hold values from -6 to 6
- norm_gain: float32 [1024], replicated, may hold values from 0.1 to 1.9
- routes: int32 [2048, 6], P(('grp', 'ep')), parts along dimension 0, may hold values from 0 to 15, all different within a row; in each aligned block of 64 rows (0 to 63, 64 to 127, ...) at most 32 rows name the same one
- gate_weights: float32 [2048, 6], P(('grp', 'ep')), parts along dimension 0, may hold values from 0.1 to 1
- w_gate: bfloat16 [16, 1024, 2048], P('ep', None, 'tp'), may hold values from -0.1875 to 0.1875
- w_up: bfloat16 [16, 1024, 2048], P('ep', None, 'tp'), may hold values from -0.1875 to 0.1875
- w_down: bfloat16 [16, 2048, 1024], P('ep', 'tp'), may hold values from -0.125 to 0.125
Outputs:
- mixed: bfloat16 [2048, 1024], P(('grp', 'ep')), parts along dimension 0
The draws below stay inside these ranges and needn't reach their ends.
There are 2 independent parts, one for each index of `grp`. The reference program is written for one: setup_inputs(seed, part) draws one part's arguments, and reference() takes and returns one part's arrays. A program takes and returns all parts, laid end to end along the dimension named above; an argument that names none is the same for every part. Nothing has to cross between parts.
Inputs may be any that keep to these rules, and one draw needn't show every extreme that they name: `routes`: each row names 6 different experts. Within the rows of one index of ep no expert is named more than 32 times, and in every draw some expert is named exactly 32 times in some index's rows.
All inputs are finite; a program needn't handle non-finite values.
Results may differ from the reference program's by a relative error of at most 0.013.
Values may be sent and summed in bfloat16 or wider, within the bound.
No kernel may reach another device: no remote copies, remote signals or barrier semaphores. Data moves between devices by JAX's collectives and lax.ppermute only.
A program may use at most 64 MiB of HBM per device.

```python
import math
import jax
import jax.numpy as jnp
import numpy as np
from jax import lax

D = 1024
FF = 2048
TOPK = 6
TOK_DEV = 64
EXPERTS = 16
CAP = 32
TOKENS = 1024
N_EP = 16
N_TP = 1


def levels(own_key, extent, shards, smallest, high):
    def one(position, parts):
        steps = jax.random.uniform(jax.random.fold_in(jax.random.fold_in(own_key, 6), position), (parts,), jnp.float32, smallest / len(shards), high / len(shards))
        return jnp.repeat(jnp.exp(steps), extent[position] // parts).reshape((-1,) + (1,) * (len(extent) - position - 1))

    level = one(*shards[0])
    for cut in shards[1:]:
        level = level * one(*cut)
    return level


def deal_out(own_key, own, number, rows, count, top, reach, slope):
    ranking = jax.random.permutation(own_key, count)
    packed, usual = portions_of(count, rows * top, reach, slope, True), portions_of(count, rows * top, reach, slope, False)
    places = jnp.arange(count)

    def named(lengths, rotation):
        used = int((lengths > 0).sum())
        fixed = max(1, used // 4)
        passed = fixed + (places - fixed + rotation * (used - fixed)) % max(1, count - fixed)
        return jnp.zeros((count,), jnp.int32).at[ranking[jnp.where(places < fixed, places, passed)]].set(jnp.asarray(lengths, jnp.int32))

    lengths = jnp.where(number % 4 == 0, named(packed, number // 4), named(usual, number - number // 4 - 1))
    mixed = jax.random.permutation(jax.random.fold_in(own, 3), count)
    source_of, taker = mixed[0:count // 2 * 2:2], mixed[1:count // 2 * 2:2]
    room = jnp.minimum(lengths[source_of] - 1, reach - lengths[taker]) // 2
    room = jnp.where((source_of == ranking[0]) | (taker == ranking[0]) | (lengths[taker] == 0), 0, jnp.maximum(room, 0))
    passed = jax.random.randint(jax.random.fold_in(own, 4), (count // 2,), 0, 1 << 20) % (room + 1)
    lengths = lengths.at[source_of].add(-passed).at[taker].add(passed)
    members = jnp.searchsorted(jnp.cumsum(lengths), jnp.arange(rows * top), side="right").astype(jnp.int32)
    table = members.reshape(top, rows).T
    table = table[jax.random.permutation(jax.random.fold_in(own, 1), rows)]
    rotation = jax.random.randint(jax.random.fold_in(own, 2), (rows, 1), 0, top)
    return jnp.take_along_axis(table, (jnp.arange(top)[None, :] + rotation) % top, axis=1)


def portions_of(number_of, total, most, skew, full):
    loads = [(1 << 20) // math.isqrt(standing ** skew) + 1 for standing in range(1, number_of + 1)]
    largest = most if full else min(most, max(-(-total // number_of), total * loads[0] // sum(loads)))
    least = 1 if total - largest >= number_of - 1 else 0
    given, rest = [largest] + [least] * (number_of - 1), total - largest - least * (number_of - 1)
    while rest > 0:
        candidates = [i for i in range(1, number_of) if given[i] < largest] or [i for i in range(1, number_of) if given[i] < most]
        whole, left = sum([loads[i] for i in candidates]), rest
        for i in candidates:
            addition = min(most - given[i], max(1, left * loads[i] // whole), rest)
            given[i] = given[i] + addition
            rest = rest - addition
    return np.array(given)


def centred(rng, extent, width, limit, shards=(), kind=jnp.bfloat16):
    array = jax.random.normal(rng, extent, jnp.float32) * width
    if len(shards) > 0:
        array = levels(rng, extent, shards, -0.22, 0.18) * array
    return jnp.clip(array, min=-limit, max=limit).astype(kind)


def setup_inputs(seed: int = 0, part: int = 0) -> dict:
    key_of = jax.random.split(jax.random.key(seed), 8)
    part_keys = jax.random.split(jax.random.fold_in(key_of[7], part), 8)
    tokens = centred(part_keys[0], (TOKENS, D), 1.0, 6.0, ((0, 16),))
    norm_gain = jnp.clip(1.0 + 0.18 * jax.random.normal(key_of[1], (D,), jnp.float32), 0.1, 1.9)
    routes_keys = jax.random.split(jax.random.fold_in(part_keys[2], 1), TOKENS // TOK_DEV)
    routes_turns = jax.random.permutation(jax.random.fold_in(part_keys[2], 3), TOKENS // TOK_DEV)
    routes = jax.vmap(lambda own, number: deal_out(jax.random.fold_in(part_keys[2], 2), own, number, TOK_DEV, EXPERTS, TOPK, CAP, 2))(routes_keys, routes_turns).reshape((TOKENS, TOPK))
    gate_weights = jnp.clip(jnp.exp(math.log(1.0) - 2.3025851 * jax.random.uniform(part_keys[3], (TOKENS, TOPK), jnp.float32) ** levels(part_keys[3], (TOKENS, TOPK), ((0, 16),), -0.2, 0.2)), 0.1, 1.0)
    w_gate = centred(key_of[4], (EXPERTS, D, FF), D ** -0.5, 0.1875, ((0, 16),))
    w_up = centred(key_of[5], (EXPERTS, D, FF), D ** -0.5, 0.1875, ((0, 16),))
    w_down = centred(key_of[6], (EXPERTS, FF, D), FF ** -0.5, 0.125, ((0, 16),))
    return dict(tokens=tokens, norm_gain=norm_gain, routes=routes, gate_weights=gate_weights, w_gate=w_gate, w_up=w_up, w_down=w_down)


def reference(tokens, norm_gain, routes, gate_weights, w_gate, w_up, w_down):
    values = tokens.astype(jnp.float32)
    scale = lax.rsqrt(lax.optimization_barrier(jnp.mean(values * values, axis=-1, keepdims=True)) + 1e-06)
    normed = (values * scale * norm_gain).astype(jnp.bfloat16)
    half = FF // N_TP
    most = CAP * N_EP

    def serve(total, expert):
        match = routes == expert
        chosen = jnp.any(match, axis=1)
        weight = lax.optimization_barrier(jnp.sum(jnp.where(match, gate_weights, 0.0), axis=1))
        index = jnp.nonzero(chosen, size=most, fill_value=0)[0].astype(jnp.int32)
        valid = (jnp.arange(most, dtype=jnp.int32) < jnp.sum(chosen.astype(jnp.int32))).astype(jnp.float32)
        rows = normed[index]
        gate = jnp.dot(rows, w_gate[expert], preferred_element_type=jnp.float32)
        up = jnp.dot(rows, w_up[expert], preferred_element_type=jnp.float32)
        hidden = (jax.nn.silu(gate) * up).astype(jnp.bfloat16)
        summed = jnp.zeros((most, D), jnp.float32)
        for block in range(N_TP):
            partial_value = jnp.dot(hidden[:, block * half:(block + 1) * half], w_down[expert][block * half:(block + 1) * half], preferred_element_type=jnp.float32).astype(jnp.bfloat16)
            summed = summed + lax.optimization_barrier(partial_value).astype(jnp.float32)
        result = lax.optimization_barrier(summed.astype(jnp.bfloat16)).astype(jnp.float32)
        term = result * (weight[index] * valid)[:, None]
        return (total.at[index].add(term), None)
    total = jnp.zeros((tokens.shape[0], D), jnp.float32)
    total, _ = lax.scan(serve, total, jnp.arange(EXPERTS, dtype=jnp.int32))
    return total.astype(jnp.bfloat16)
```

```python
import jax
import jax.numpy as jnp
from jax import lax
from jax.sharding import PartitionSpec as P


def shards(tokens, norm_gain, routes, gate_weights, w_gate, w_up, w_down):
    values = tokens.astype(jnp.float32)
    scale = lax.rsqrt(jnp.mean(values * values, axis=-1, keepdims=True) + 1e-06)
    normed = (values * scale * norm_gain).astype(jnp.bfloat16)
    width = tokens.shape[1]
    tok_dev = tokens.shape[0]
    topk = routes.shape[1]
    experts = lax.axis_size("ep")
    capacity = min(tok_dev, max(2, 4 * tok_dev * topk // (3 * experts)))
    slots = capacity * experts
    me = lax.axis_index("ep")
    all_normed = lax.all_gather(normed, "ep", axis=0, tiled=True)
    hits = routes[:, :, None] == jnp.arange(experts, dtype=jnp.int32)[None, None, :]
    weight_tok = jnp.sum(jnp.where(hits, gate_weights[:, :, None], 0.0), axis=1)
    weights_t = lax.all_to_all(weight_tok.T, "ep", split_axis=0, concat_axis=0, tiled=True)
    chosen = weights_t > 0.0
    lower = (jnp.arange(tok_dev)[:, None] < jnp.arange(tok_dev)[None, :]).astype(jnp.bfloat16)
    rank = jnp.dot(chosen.astype(jnp.bfloat16), lower, preferred_element_type=jnp.float32)
    base = jnp.arange(experts, dtype=jnp.int32)[:, None] * capacity
    slot = jnp.where(chosen, rank.astype(jnp.int32) + base, -1).reshape(1, -1)
    placed = slot == jnp.arange(slots, dtype=jnp.int32)[:, None]
    place = placed.astype(jnp.bfloat16)
    weight = jnp.sum(jnp.where(placed, weights_t.reshape(1, -1), 0.0), axis=1, keepdims=True)
    rows = jnp.dot(place, all_normed, preferred_element_type=jnp.float32).astype(jnp.bfloat16)
    gate = jnp.dot(rows, w_gate[0], preferred_element_type=jnp.float32)
    up = jnp.dot(rows, w_up[0], preferred_element_type=jnp.float32)
    hidden = (jax.nn.silu(gate) * up).astype(jnp.bfloat16)
    output = jnp.dot(hidden, w_down[0], preferred_element_type=jnp.float32).astype(jnp.bfloat16)
    output = lax.psum(output, "tp")
    terms = (output.astype(jnp.float32) * weight).astype(jnp.bfloat16)
    spread = jnp.dot(place.T, terms, preferred_element_type=jnp.float32).astype(jnp.bfloat16)
    return lax.psum_scatter(spread, "ep", scatter_dimension=0, tiled=True)


def solution(mesh):
    in_specs = (
        P(("grp", "ep"), None),
        P(),
        P(("grp", "ep"), None),
        P(("grp", "ep"), None),
        P("ep", None, "tp"),
        P("ep", None, "tp"),
        P("ep", "tp", None),
    )
    out_specs = P(("grp", "ep"), None)
    return jax.shard_map(shards, mesh=mesh, in_specs=in_specs, out_specs=out_specs, check_vma=False)
```

```python
import functools

import jax
import jax.numpy as jnp
from jax import lax
from jax.experimental import pallas as pl
from jax.experimental.pallas import tpu as pltpu
from jax.sharding import PartitionSpec as P

LANES = 128


def prepare(tokens_ref, gain_ref, routes_ref, weights_ref, out_ref, *, experts):
    rows, width = tokens_ref.shape
    values = tokens_ref[...].astype(jnp.float32)
    scale = lax.rsqrt(jnp.mean(values * values, axis=-1, keepdims=True) + 1e-06)
    out_ref[:, :width] = (values * scale * gain_ref[...]).astype(jnp.bfloat16)
    table = out_ref.shape[1] - width
    lane = lax.broadcasted_iota(jnp.int32, (rows, table), 1)
    expert = lane % experts
    weight = jnp.zeros((rows, table), jnp.float32)
    chosen = jnp.zeros((rows, table), jnp.float32)
    for j in range(routes_ref.shape[1]):
        hit = routes_ref[:, j:j + 1] == expert
        weight = weight + jnp.where(hit, weights_ref[:, j:j + 1], 0.0)
        chosen = chosen + jnp.where(hit, 1.0, 0.0)
    earlier = lax.broadcasted_iota(jnp.int32, (rows, rows), 0) > lax.broadcasted_iota(jnp.int32, (rows, rows), 1)
    earlier = jnp.where(earlier, 1.0, 0.0).astype(jnp.bfloat16)
    rank = jnp.dot(earlier, chosen.astype(jnp.bfloat16), preferred_element_type=jnp.float32)
    upper = weight.astype(jnp.bfloat16).astype(jnp.float32)
    packed = jnp.where(lane < 3 * experts, weight - upper, 0.0)
    packed = jnp.where(lane < 2 * experts, upper, packed)
    packed = jnp.where(lane < experts, jnp.where(chosen > 0.0, rank, -1.0), packed)
    out_ref[:, width:] = packed.astype(jnp.bfloat16)


def serve(me_ref, *refs, blocks, experts, capacity, width, pieces):
    block_refs = refs[:blocks]
    gate_hbm, up_hbm, down_hbm = refs[blocks:blocks + 3]
    quads = blocks // 4
    outs = refs[blocks + 3:blocks + 3 + 2 * quads]
    gate_v, up_v, down_v, rows_v, hidden_v, sems = refs[blocks + 3 + 2 * quads:]
    ff = gate_v.shape[1]
    cut = ff // pieces
    copies = []
    for p in range(pieces):
        span = pl.ds(p * cut, cut)
        copies.append((
            pltpu.make_async_copy(gate_hbm.at[:, span], gate_v.at[:, span], sems.at[0, p]),
            pltpu.make_async_copy(up_hbm.at[:, span], up_v.at[:, span], sems.at[1, p]),
        ))
    down_copy = pltpu.make_async_copy(down_hbm, down_v, sems.at[2, 0])
    for pair in copies:
        for copy in pair:
            copy.start()
    down_copy.start()
    me = me_ref[0]
    tok = block_refs[0].shape[0]
    table = block_refs[0].shape[1] - width
    slots = 4 * capacity
    own = lax.broadcasted_iota(jnp.int32, (8, table), 1) == me
    own = jnp.where(own, 1.0, 0.0).astype(jnp.bfloat16)
    slot_lane = lax.broadcasted_iota(jnp.int32, (slots, table), 1)
    token_lane = lax.broadcasted_iota(jnp.int32, (4 * tok, table), 1)
    spread_of, weight_of = [], []
    for q in range(quads):
        order = [4 * q, 4 * q + 2, 4 * q + 1, 4 * q + 3]
        data = jnp.concatenate([block_refs[k][:, :width] for k in order], axis=0)
        tab = jnp.concatenate([block_refs[k][:, width:] for k in order], axis=0)
        row = lax.dot_general(own, tab, (((1,), (1,)), ((), ())), preferred_element_type=jnp.float32)[0:1]
        base = (lax.broadcasted_iota(jnp.int32, (1, 4 * tok), 1) // tok * capacity).astype(jnp.float32)
        slot_row = jnp.where(row >= 0.0, row + base, -1.0)
        place = slot_row == lax.broadcasted_iota(jnp.int32, (slots, 4 * tok), 0).astype(jnp.float32)
        place = jnp.where(place, 1.0, 0.0).astype(jnp.bfloat16)
        rows_v[q * slots:(q + 1) * slots, :] = jnp.dot(place, data, preferred_element_type=jnp.float32).astype(jnp.bfloat16)
        entries = jnp.dot(place, tab, preferred_element_type=jnp.float32)
        mine = (slot_lane == experts + me) | (slot_lane == 2 * experts + me)
        weight_of.append(jnp.sum(jnp.where(mine, entries, 0.0), axis=1, keepdims=True))
        column = jnp.sum(jnp.where(token_lane == me, tab.astype(jnp.float32), 0.0), axis=1, keepdims=True)
        base = (lax.broadcasted_iota(jnp.int32, (4 * tok, 1), 0) // tok * capacity).astype(jnp.float32)
        slot_col = jnp.where(column >= 0.0, column + base, -1.0)
        spread = slot_col == lax.broadcasted_iota(jnp.int32, (4 * tok, slots), 1).astype(jnp.float32)
        spread_of.append(jnp.where(spread, 1.0, 0.0).astype(jnp.bfloat16))
    for p in range(pieces):
        for copy in copies[p]:
            copy.wait()
        span = slice(p * cut, (p + 1) * cut)
        gate = jnp.dot(rows_v[...], gate_v[:, span], preferred_element_type=jnp.float32)
        up = jnp.dot(rows_v[...], up_v[:, span], preferred_element_type=jnp.float32)
        hidden_v[:, span] = (gate / (1.0 + jnp.exp(-gate)) * up).astype(jnp.bfloat16)
    down_copy.wait()
    for q in range(quads):
        out = jnp.dot(hidden_v[q * slots:(q + 1) * slots, :], down_v[...], preferred_element_type=jnp.float32)
        out = out.astype(jnp.bfloat16).astype(jnp.float32)
        terms = (out * weight_of[q]).astype(jnp.bfloat16)
        result = jnp.dot(spread_of[q], terms, preferred_element_type=jnp.float32).astype(jnp.bfloat16)
        outs[2 * q][...] = result[:2 * tok]
        outs[2 * q + 1][...] = result[2 * tok:]


def add(a, b):
    return (a.astype(jnp.float32) + b.astype(jnp.float32)).astype(jnp.bfloat16)


def shards(tokens, norm_gain, routes, gate_weights, w_gate, w_up, w_down):
    tok, width = tokens.shape
    topk = routes.shape[1]
    experts = lax.axis_size("ep")
    capacity = min(tok, max(2, 4 * tok * topk // (3 * experts)))
    ff = w_gate.shape[2]
    quads = experts // 4
    table = -(-3 * experts // LANES) * LANES

    def swap(x, k):
        return lax.ppermute(x, "ep", [(e, e ^ k) for e in range(experts)])

    mine = pl.pallas_call(
        functools.partial(prepare, experts=experts),
        out_shape=jax.ShapeDtypeStruct((tok, width + table), jnp.bfloat16),
    )(tokens, norm_gain.reshape(1, -1), routes, gate_weights)
    blocks = {0: mine}
    for q in range(1, quads):
        blocks[4 * q] = swap(mine, 4 * q)
    for q in range(quads):
        blocks[4 * q + 2] = swap(blocks[4 * q], 2)
    for q in range(quads):
        blocks[4 * q + 1] = swap(blocks[4 * q], 1)
        blocks[4 * q + 3] = swap(blocks[4 * q + 2], 1)
    me = lax.axis_index("ep").reshape(1).astype(jnp.int32)
    half = jax.ShapeDtypeStruct((2 * tok, width), jnp.bfloat16)
    vmem = pl.BlockSpec(memory_space=pltpu.VMEM)
    pieces = 4
    outs = pl.pallas_call(
        functools.partial(serve, blocks=experts, experts=experts, capacity=capacity, width=width, pieces=pieces),
        out_shape=[half] * (2 * quads),
        in_specs=[pl.BlockSpec(memory_space=pltpu.SMEM)] + [vmem] * experts + [pl.BlockSpec(memory_space=pl.ANY)] * 3,
        out_specs=[vmem] * (2 * quads),
        scratch_shapes=[
            pltpu.VMEM((width, ff), jnp.bfloat16),
            pltpu.VMEM((width, ff), jnp.bfloat16),
            pltpu.VMEM((ff, width), jnp.bfloat16),
            pltpu.VMEM((experts * capacity, width), jnp.bfloat16),
            pltpu.VMEM((experts * capacity, ff), jnp.bfloat16),
            pltpu.SemaphoreType.DMA((3, pieces)),
        ],
        compiler_params=pltpu.CompilerParams(vmem_limit_bytes=40 * 1024 * 1024),
    )(me, *[blocks[k] for k in range(experts)], w_gate[0], w_up[0], w_down[0])
    if lax.axis_size("tp") > 1:
        outs = [lax.psum(o, "tp") for o in outs]
    total = None
    for q in range(quads):
        kept = add(outs[2 * q], swap(outs[2 * q + 1], 1))
        kept = add(kept[:tok], swap(kept[tok:], 2))
        if q:
            kept = swap(kept, 4 * q)
        kept = kept.astype(jnp.float32)
        total = kept if total is None else total + kept
    return total.astype(jnp.bfloat16)


def solution(mesh):
    in_specs = (
        P(("grp", "ep"), None),
        P(),
        P(("grp", "ep"), None),
        P(("grp", "ep"), None),
        P("ep", None, "tp"),
        P("ep", None, "tp"),
        P("ep", "tp", None),
    )
    out_specs = P(("grp", "ep"), None)
    return jax.shard_map(shards, mesh=mesh, in_specs=in_specs, out_specs=out_specs, check_vma=False)
```

```python
import functools

import jax
import jax.numpy as jnp
from jax import lax
from jax.experimental import pallas as pl
from jax.experimental.pallas import tpu as pltpu
from jax.sharding import PartitionSpec as P

LANES = 128


def prepare(tokens_ref, gain_ref, routes_ref, weights_ref, out_ref, *, experts):
    rows, width = tokens_ref.shape
    values = tokens_ref[...].astype(jnp.float32)
    scale = lax.rsqrt(jnp.mean(values * values, axis=-1, keepdims=True) + 1e-06)
    out_ref[:, :width] = (values * scale * gain_ref[...]).astype(jnp.bfloat16)
    table = out_ref.shape[1] - width
    lane = lax.broadcasted_iota(jnp.int32, (rows, table), 1)
    expert = lane % experts
    weight = jnp.zeros((rows, table), jnp.float32)
    chosen = jnp.zeros((rows, table), jnp.float32)
    routes = routes_ref[...].T
    gates = weights_ref[...].T
    for j in range(routes_ref.shape[0]):
        hit = routes[:, j:j + 1] == expert
        weight = weight + jnp.where(hit, gates[:, j:j + 1], 0.0)
        chosen = chosen + jnp.where(hit, 1.0, 0.0)
    earlier = lax.broadcasted_iota(jnp.int32, (rows, rows), 0) > lax.broadcasted_iota(jnp.int32, (rows, rows), 1)
    earlier = jnp.where(earlier, 1.0, 0.0).astype(jnp.bfloat16)
    rank = jnp.dot(earlier, chosen.astype(jnp.bfloat16), preferred_element_type=jnp.float32)
    upper = weight.astype(jnp.bfloat16).astype(jnp.float32)
    packed = jnp.where(lane < 3 * experts, weight - upper, 0.0)
    packed = jnp.where(lane < 2 * experts, upper, packed)
    packed = jnp.where(lane < experts, jnp.where(chosen > 0.0, rank, -1.0), packed)
    out_ref[:, width:] = packed.astype(jnp.bfloat16)


def serve(me_ref, *refs, quads, experts, capacity, width, pieces, loads):
    block_refs = refs[:4 * quads]
    weights = refs[4 * quads:4 * quads + 3]
    rest = refs[4 * quads + 3:]
    outs, rest = rest[:2 * quads], rest[2 * quads:]
    copies = []
    if loads:
        (gate_v, up_v, down_v), (rows_v, hidden_v, sems) = rest[:3], rest[3:]
        cut = gate_v.shape[1] // pieces
        for p in range(pieces):
            span = pl.ds(p * cut, cut)
            copies.append([
                pltpu.make_async_copy(weights[w].at[:, span], rest[w].at[:, span], sems.at[w, p])
                for w in range(2)
            ])
        copies.append([pltpu.make_async_copy(weights[2], down_v, sems.at[2, 0])])
        for group in copies:
            for copy in group:
                copy.start()
    else:
        (gate_v, up_v, down_v), (rows_v, hidden_v) = weights, rest
        cut = gate_v.shape[1] // pieces
    me = me_ref[0]
    tok = block_refs[0].shape[0]
    table = block_refs[0].shape[1] - width
    slots = 4 * capacity
    own = lax.broadcasted_iota(jnp.int32, (8, table), 1) == me
    own = jnp.where(own, 1.0, 0.0).astype(jnp.bfloat16)
    slot_lane = lax.broadcasted_iota(jnp.int32, (slots, table), 1)
    token_lane = lax.broadcasted_iota(jnp.int32, (4 * tok, table), 1)
    spread_of, weight_of = [], []
    for q in range(quads):
        order = [4 * q, 4 * q + 2, 4 * q + 1, 4 * q + 3]
        data = jnp.concatenate([block_refs[k][:, :width] for k in order], axis=0)
        tab = jnp.concatenate([block_refs[k][:, width:] for k in order], axis=0)
        row = lax.dot_general(own, tab, (((1,), (1,)), ((), ())), preferred_element_type=jnp.float32)[0:1]
        base = (lax.broadcasted_iota(jnp.int32, (1, 4 * tok), 1) // tok * capacity).astype(jnp.float32)
        slot_row = jnp.where(row >= 0.0, row + base, -1.0)
        place = slot_row == lax.broadcasted_iota(jnp.int32, (slots, 4 * tok), 0).astype(jnp.float32)
        place = jnp.where(place, 1.0, 0.0).astype(jnp.bfloat16)
        rows_v[q * slots:(q + 1) * slots, :] = jnp.dot(place, data, preferred_element_type=jnp.float32).astype(jnp.bfloat16)
        entries = jnp.dot(place, tab, preferred_element_type=jnp.float32)
        mine = (slot_lane == experts + me) | (slot_lane == 2 * experts + me)
        weight_of.append(jnp.sum(jnp.where(mine, entries, 0.0), axis=1, keepdims=True))
        column = jnp.sum(jnp.where(token_lane == me, tab.astype(jnp.float32), 0.0), axis=1, keepdims=True)
        base = (lax.broadcasted_iota(jnp.int32, (4 * tok, 1), 0) // tok * capacity).astype(jnp.float32)
        slot_col = jnp.where(column >= 0.0, column + base, -1.0)
        spread = slot_col == lax.broadcasted_iota(jnp.int32, (4 * tok, slots), 1).astype(jnp.float32)
        spread_of.append(jnp.where(spread, 1.0, 0.0).astype(jnp.bfloat16))
    for p in range(pieces):
        if loads:
            for copy in copies[p]:
                copy.wait()
        span = slice(p * cut, (p + 1) * cut)
        gate = jnp.dot(rows_v[...], gate_v[:, span], preferred_element_type=jnp.float32)
        up = jnp.dot(rows_v[...], up_v[:, span], preferred_element_type=jnp.float32)
        hidden_v[:, span] = (gate / (1.0 + jnp.exp(-gate)) * up).astype(jnp.bfloat16)
    if loads:
        copies[pieces][0].wait()
    out = jnp.dot(hidden_v[...], down_v[...], preferred_element_type=jnp.float32)
    out = out.astype(jnp.bfloat16).astype(jnp.float32)
    for q in range(quads):
        terms = (out[q * slots:(q + 1) * slots] * weight_of[q]).astype(jnp.bfloat16)
        result = jnp.dot(spread_of[q], terms, preferred_element_type=jnp.float32).astype(jnp.bfloat16)
        outs[2 * q][...] = result[:2 * tok]
        outs[2 * q + 1][...] = result[2 * tok:]


def add(a, b):
    return (a.astype(jnp.float32) + b.astype(jnp.float32)).astype(jnp.bfloat16)


def shards(tokens, norm_gain, routes, gate_weights, w_gate, w_up, w_down):
    tok, width = tokens.shape
    topk = routes.shape[1]
    experts = lax.axis_size("ep")
    capacity = min(tok, max(2, 4 * tok * topk // (3 * experts)))
    ff = w_gate.shape[2]
    quads = experts // 4
    table = -(-3 * experts // LANES) * LANES

    def swap(x, k):
        return lax.ppermute(x, "ep", [(e, e ^ k) for e in range(experts)])

    mine = pl.pallas_call(
        functools.partial(prepare, experts=experts),
        out_shape=jax.ShapeDtypeStruct((tok, width + table), jnp.bfloat16),
    )(tokens, norm_gain.reshape(1, -1), routes.T, gate_weights.T)
    blocks = {0: mine}
    for q in range(1, quads):
        blocks[4 * q] = swap(mine, 4 * q)
    for q in range(quads):
        blocks[4 * q + 2] = swap(blocks[4 * q], 2)
    for q in range(quads):
        blocks[4 * q + 1] = swap(blocks[4 * q], 1)
        blocks[4 * q + 3] = swap(blocks[4 * q + 2], 1)
    me = lax.axis_index("ep").reshape(1).astype(jnp.int32)
    half = jax.ShapeDtypeStruct((2 * tok, width), jnp.bfloat16)
    vmem = pl.BlockSpec(memory_space=pltpu.VMEM)
    pieces = 4
    group = quads // 2

    def run(first, weights, loads):
        held = [jax.ShapeDtypeStruct(w.shape, w.dtype) for w in weights] if loads else []
        scratch = [
            pltpu.VMEM((group * 4 * capacity, width), jnp.bfloat16),
            pltpu.VMEM((group * 4 * capacity, ff), jnp.bfloat16),
        ]
        if loads:
            scratch.append(pltpu.SemaphoreType.DMA((3, pieces)))
        source = pl.BlockSpec(memory_space=pltpu.HBM) if loads else vmem
        return pl.pallas_call(
            functools.partial(serve, quads=group, experts=experts, capacity=capacity, width=width, pieces=pieces, loads=loads),
            out_shape=[half] * (2 * group) + held,
            in_specs=[pl.BlockSpec(memory_space=pltpu.SMEM)] + [vmem] * (4 * group) + [source] * 3,
            out_specs=[vmem] * (2 * group + len(held)),
            scratch_shapes=scratch,
            compiler_params=pltpu.CompilerParams(vmem_limit_bytes=16 * 1024 * 1024),
            name="near" if loads else "far",
        )(me, *[blocks[4 * first + k] for k in range(4 * group)], *weights)

    near = run(0, (w_gate[0], w_up[0], w_down[0]), True)
    far = run(group, near[2 * group:], False)
    outs = list(near[:2 * group]) + list(far)
    if lax.axis_size("tp") > 1:
        outs = [lax.psum(o, "tp") for o in outs]
    total = None
    for q in range(quads):
        kept = add(outs[2 * q], swap(outs[2 * q + 1], 1))
        kept = add(kept[:tok], swap(kept[tok:], 2))
        if q:
            kept = swap(kept, 4 * q)
        kept = kept.astype(jnp.float32)
        total = kept if total is None else total + kept
    return total.astype(jnp.bfloat16)


def solution(mesh):
    in_specs = (
        P(("grp", "ep"), None),
        P(),
        P(("grp", "ep"), None),
        P(("grp", "ep"), None),
        P("ep", None, "tp"),
        P("ep", None, "tp"),
        P("ep", "tp", None),
    )
    out_specs = P(("grp", "ep"), None)
    return jax.shard_map(shards, mesh=mesh, in_specs=in_specs, out_specs=out_specs, check_vma=False)
```

```python
import functools

import jax
import jax.numpy as jnp
from jax import lax
from jax.experimental import pallas as pl
from jax.experimental.pallas import tpu as pltpu
from jax.sharding import PartitionSpec as P

LANES = 128


def prepare(tokens_ref, gain_ref, routes_ref, weights_ref, out_ref, *, experts):
    rows, width = tokens_ref.shape
    values = tokens_ref[...].astype(jnp.float32)
    scale = lax.rsqrt(jnp.mean(values * values, axis=-1, keepdims=True) + 1e-06)
    out_ref[:, :width] = (values * scale * gain_ref[...]).astype(jnp.bfloat16)
    table = out_ref.shape[1] - width
    lane = lax.broadcasted_iota(jnp.int32, (rows, table), 1)
    expert = lane % experts
    weight = jnp.zeros((rows, table), jnp.float32)
    chosen = jnp.zeros((rows, table), jnp.float32)
    routes = routes_ref[...].T
    gates = weights_ref[...].T
    for j in range(routes_ref.shape[0]):
        hit = routes[:, j:j + 1] == expert
        weight = weight + jnp.where(hit, gates[:, j:j + 1], 0.0)
        chosen = chosen + jnp.where(hit, 1.0, 0.0)
    earlier = lax.broadcasted_iota(jnp.int32, (rows, rows), 0) > lax.broadcasted_iota(jnp.int32, (rows, rows), 1)
    earlier = jnp.where(earlier, 1.0, 0.0).astype(jnp.bfloat16)
    rank = jnp.dot(earlier, chosen.astype(jnp.bfloat16), preferred_element_type=jnp.float32)
    upper = weight.astype(jnp.bfloat16).astype(jnp.float32)
    packed = jnp.where(lane < 3 * experts, weight - upper, 0.0)
    packed = jnp.where(lane < 2 * experts, upper, packed)
    packed = jnp.where(lane < experts, jnp.where(chosen > 0.0, rank, -1.0), packed)
    out_ref[:, width:] = packed.astype(jnp.bfloat16)


def serve(me_ref, *refs, quads, experts, capacity, width, pieces, loads):
    block_refs = refs[:4 * quads]
    weights = refs[4 * quads:4 * quads + 3]
    rest = refs[4 * quads + 3:]
    outs, rest = rest[:2 * quads], rest[2 * quads:]
    copies = []
    if loads:
        (gate_v, up_v, down_v), (rows_v, hidden_v, sems) = rest[:3], rest[3:]
        cut = gate_v.shape[1] // pieces
        for p in range(pieces):
            span = pl.ds(p * cut, cut)
            copies.append([
                pltpu.make_async_copy(weights[w].at[:, span], rest[w].at[:, span], sems.at[w, p])
                for w in range(2)
            ])
        copies.append([pltpu.make_async_copy(weights[2], down_v, sems.at[2, 0])])
        for group in copies:
            for copy in group:
                copy.start()
    else:
        (gate_v, up_v, down_v), (rows_v, hidden_v) = weights, rest
        cut = gate_v.shape[1] // pieces
    me = me_ref[0]
    tok = block_refs[0].shape[0]
    table = block_refs[0].shape[1] - width
    slots = 4 * capacity
    own = lax.broadcasted_iota(jnp.int32, (8, table), 1) == me
    own = jnp.where(own, 1.0, 0.0).astype(jnp.bfloat16)
    slot_lane = lax.broadcasted_iota(jnp.int32, (slots, table), 1)
    token_lane = lax.broadcasted_iota(jnp.int32, (4 * tok, table), 1)
    spread_of, weight_of = [], []
    for q in range(quads):
        order = [4 * q, 4 * q + 2, 4 * q + 1, 4 * q + 3]
        data = jnp.concatenate([block_refs[k][:, :width] for k in order], axis=0)
        tab = jnp.concatenate([block_refs[k][:, width:] for k in order], axis=0)
        row = lax.dot_general(own, tab, (((1,), (1,)), ((), ())), preferred_element_type=jnp.float32)[0:1]
        base = (lax.broadcasted_iota(jnp.int32, (1, 4 * tok), 1) // tok * capacity).astype(jnp.float32)
        slot_row = jnp.where(row >= 0.0, row + base, -1.0)
        place = slot_row == lax.broadcasted_iota(jnp.int32, (slots, 4 * tok), 0).astype(jnp.float32)
        place = jnp.where(place, 1.0, 0.0).astype(jnp.bfloat16)
        rows_v[q * slots:(q + 1) * slots, :] = jnp.dot(place, data, preferred_element_type=jnp.float32).astype(jnp.bfloat16)
        entries = jnp.dot(place, tab, preferred_element_type=jnp.float32)
        mine = (slot_lane == experts + me) | (slot_lane == 2 * experts + me)
        weight_of.append(jnp.sum(jnp.where(mine, entries, 0.0), axis=1, keepdims=True))
        column = jnp.sum(jnp.where(token_lane == me, tab.astype(jnp.float32), 0.0), axis=1, keepdims=True)
        base = (lax.broadcasted_iota(jnp.int32, (4 * tok, 1), 0) // tok * capacity).astype(jnp.float32)
        slot_col = jnp.where(column >= 0.0, column + base, -1.0)
        spread = slot_col == lax.broadcasted_iota(jnp.int32, (4 * tok, slots), 1).astype(jnp.float32)
        spread_of.append(jnp.where(spread, 1.0, 0.0).astype(jnp.bfloat16))
    for p in range(pieces):
        if loads:
            for copy in copies[p]:
                copy.wait()
        span = slice(p * cut, (p + 1) * cut)
        gate = jnp.dot(rows_v[...], gate_v[:, span], preferred_element_type=jnp.float32)
        up = jnp.dot(rows_v[...], up_v[:, span], preferred_element_type=jnp.float32)
        hidden_v[:, span] = (gate / (1.0 + jnp.exp(-gate)) * up).astype(jnp.bfloat16)
    if loads:
        copies[pieces][0].wait()
    out = jnp.dot(hidden_v[...], down_v[...], preferred_element_type=jnp.float32)
    out = out.astype(jnp.bfloat16).astype(jnp.float32)
    for q in range(quads):
        terms = (out[q * slots:(q + 1) * slots] * weight_of[q]).astype(jnp.bfloat16)
        result = jnp.dot(spread_of[q], terms, preferred_element_type=jnp.float32).astype(jnp.bfloat16)
        outs[2 * q][...] = result[:2 * tok]
        outs[2 * q + 1][...] = result[2 * tok:]


def add(a, b):
    return (a.astype(jnp.float32) + b.astype(jnp.float32)).astype(jnp.bfloat16)


def shards(tokens, norm_gain, routes, gate_weights, w_gate, w_up, w_down):
    tok, width = tokens.shape
    topk = routes.shape[1]
    experts = lax.axis_size("ep")
    capacity = min(tok, max(2, 4 * tok * topk // (3 * experts)))
    ff = w_gate.shape[2]
    quads = experts // 4
    table = -(-3 * experts // LANES) * LANES

    def swap(x, k):
        return lax.ppermute(x, "ep", [(e, e ^ k) for e in range(experts)])

    mine = pl.pallas_call(
        functools.partial(prepare, experts=experts),
        out_shape=jax.ShapeDtypeStruct((tok, width + table), jnp.bfloat16),
    )(tokens, norm_gain.reshape(1, -1), routes.T, gate_weights.T)
    blocks = {0: mine}
    for q in range(1, quads):
        blocks[4 * q] = swap(mine, 4 * q)
    for q in range(quads):
        blocks[4 * q + 2] = swap(blocks[4 * q], 2)
    for q in range(quads):
        blocks[4 * q + 1] = swap(blocks[4 * q], 1)
        blocks[4 * q + 3] = swap(blocks[4 * q + 2], 1)
    me = lax.axis_index("ep").reshape(1).astype(jnp.int32)
    half = jax.ShapeDtypeStruct((2 * tok, width), jnp.bfloat16)
    vmem = pl.BlockSpec(memory_space=pltpu.VMEM)
    pieces = 4
    group = quads // 2

    def run(first, weights, loads):
        held = [jax.ShapeDtypeStruct(w.shape, w.dtype) for w in weights] if loads else []
        scratch = [
            pltpu.VMEM((group * 4 * capacity, width), jnp.bfloat16),
            pltpu.VMEM((group * 4 * capacity, ff), jnp.bfloat16),
        ]
        if loads:
            scratch.append(pltpu.SemaphoreType.DMA((3, pieces)))
        source = pl.BlockSpec(memory_space=pltpu.HBM) if loads else vmem
        return pl.pallas_call(
            functools.partial(serve, quads=group, experts=experts, capacity=capacity, width=width, pieces=pieces, loads=loads),
            out_shape=[half] * (2 * group) + held,
            in_specs=[pl.BlockSpec(memory_space=pltpu.SMEM)] + [vmem] * (4 * group) + [source] * 3,
            out_specs=[vmem] * (2 * group + len(held)),
            scratch_shapes=scratch,
            compiler_params=pltpu.CompilerParams(vmem_limit_bytes=16 * 1024 * 1024),
            name="near" if loads else "far",
        )(me, *[blocks[4 * first + k] for k in range(4 * group)], *weights)

    weights = [pltpu.with_memory_space_constraint(w[0], pltpu.HBM) for w in (w_gate, w_up, w_down)]
    near = run(0, weights, True)
    far = run(group, near[2 * group:], False)
    outs = list(near[:2 * group]) + list(far)
    if lax.axis_size("tp") > 1:
        outs = [lax.psum(o, "tp") for o in outs]
    total = None
    for q in range(quads):
        kept = add(outs[2 * q], swap(outs[2 * q + 1], 1))
        kept = add(kept[:tok], swap(kept[tok:], 2))
        if q:
            kept = swap(kept, 4 * q)
        kept = kept.astype(jnp.float32)
        total = kept if total is None else total + kept
    return total.astype(jnp.bfloat16)


def solution(mesh):
    in_specs = (
        P(("grp", "ep"), None),
        P(),
        P(("grp", "ep"), None),
        P(("grp", "ep"), None),
        P("ep", None, "tp"),
        P("ep", None, "tp"),
        P("ep", "tp", None),
    )
    out_specs = P(("grp", "ep"), None)
    return jax.shard_map(shards, mesh=mesh, in_specs=in_specs, out_specs=out_specs, check_vma=False)
```
